32 devices in a mesh: rep: 2 (over y), fs: 4 (over z), tp: 4 (over x, core).
Axes of the slice: x: 2, y: 2, z: 4, core: 2. Of those that a mesh axis runs over, the one named last changes fastest.
Arguments:
- tokens: bfloat16 [4096, 2048], P(('rep', 'fs'), 'tp'), may hold values from -6 to 6
- outer_gate: float32 [2048, 512], P('fs', 'tp'), may hold values from -0.125 to 0.125
- inner_gate: float32 [2048, 512], P('fs', 'tp'), may hold values from -0.125 to 0.125
- mixer_value: float32 [2048, 512], P('fs', 'tp'), may hold values from -0.125 to 0.125
- mixer_scales: float32 [3, 512], P(None, 'tp'), may hold values from 0.5 to 2
- mixer_taps: float32 [3, 512], P(None, 'tp'), may hold values from -3.5 to 3.5
- mixer_out: float32 [512, 2048], P('fs', 'tp'), may hold values from -0.25 to 0.25
- out_scale: float32 [2048], P('tp'), may hold values from 0.3 to 3
- first_gain: float32 [2048], replicated, may hold values from 0.1 to 1.9
- first_shift: float32 [2048], replicated, may hold values from -2 to 2
- up_proj: float32 [2048, 3072], P('fs', 'tp'), may hold values from -0.125 to 0.125
- gate_proj: float32 [2048, 3072], P('fs', 'tp'), may hold values from -0.125 to 0.125
- up_scales: float32 [2, 3072], P(None, 'tp'), may hold values from 0.5 to 2
- ffn_taps: float32 [3, 2, 3072], P(None, None, 'tp'), may hold values from -3.5 to 3.5
- ffn_shift: float32 [2, 3072], P(None, 'tp'), may hold values from -3 to 3
- down_proj: float32 [3072, 2048], P('fs', 'tp'), may hold values from -0.109375 to 0.109375
- down_scale: float32 [2048], P('tp'), may hold values from 0.3 to 3
- second_gain: float32 [2048], replicated, may hold values from 0.1 to 1.9
- second_shift: float32 [2048], replicated, may hold values from -2 to 2
Outputs:
- layer_out: bfloat16 [4096, 2048], P(('rep', 'fs'), 'tp')
The draws below stay inside these ranges and needn't reach their ends.
All inputs are finite; a program needn't handle non-finite values.
Results may differ from the reference program's by a relative error of at most 0.017.
Values may be sent and summed in bfloat16 or wider, within the bound.
No kernel may reach another device: no remote copies, remote signals or barrier semaphores. Data moves between devices by JAX's collectives and lax.ppermute only.
A program may use at most 64 MiB of HBM per device.

```python
import math
import jax
import jax.numpy as jnp
from jax import lax

D = 2048
CW = 512
FF = 3072
LEN = 128
TOKENS = 4096


def shard_levels(rng, shape, split, low, largest):
    def one(position, parts):
        heights = jax.random.uniform(jax.random.fold_in(jax.random.fold_in(rng, 6), position), (parts,), jnp.float32, low / len(split), largest / len(split))
        return jnp.repeat(jnp.exp(heights), shape[position] // parts).reshape((-1,) + (1,) * (len(shape) - position - 1))

    level = one(*split[0])
    for cut in split[1:]:
        level = level * one(*cut)
    return level


def centred(key, dims, width, bound, split=(), kind=jnp.bfloat16):
    array = jax.random.normal(key, dims, jnp.float32) * width
    if len(split) > 0:
        array = shard_levels(key, dims, split, -0.22, 0.18) * array
    return jnp.clip(array, min=-bound, max=bound).astype(kind)


def setup_inputs(seed: int = 0) -> dict:
    key_list = jax.random.split(jax.random.key(seed), 20)
    tokens = centred(key_list[0], (TOKENS, D), 1.0, 6.0, ((0, 8), (1, 4)))
    outer_gate = centred(key_list[1], (D, CW), D ** -0.5, 0.125, ((0, 4), (1, 4)), jnp.float32)
    inner_gate = centred(key_list[2], (D, CW), D ** -0.5, 0.125, ((0, 4), (1, 4)), jnp.float32)
    mixer_value = centred(key_list[3], (D, CW), D ** -0.5, 0.125, ((0, 4), (1, 4)), jnp.float32)
    mixer_scales = jnp.clip(jnp.exp(math.log(2.0) - 1.3862944 * jax.random.uniform(key_list[4], (3, CW), jnp.float32) ** shard_levels(key_list[4], (3, CW), ((1, 4),), -0.2, 0.2)), 0.5, 2.0)
    mixer_taps = centred(key_list[5], (3, CW), 3 ** -0.5, 3.5, ((1, 4),), jnp.float32)
    mixer_out = centred(key_list[6], (CW, D), CW ** -0.5, 0.25, ((0, 4), (1, 4)), jnp.float32)
    out_scale = jnp.clip(jnp.exp(math.log(3.0) - 2.3025851 * jax.random.uniform(key_list[7], (D,), jnp.float32) ** shard_levels(key_list[7], (D,), ((0, 4),), -0.2, 0.2)), 0.3, 3.0)
    first_gain = jnp.clip(1.0 + 0.18 * jax.random.normal(key_list[8], (D,), jnp.float32), 0.1, 1.9)
    first_shift = centred(key_list[9], (D,), 0.3, 2.0, (), jnp.float32)
    up_proj = centred(key_list[10], (D, FF), D ** -0.5, 0.125, ((0, 4), (1, 4)), jnp.float32)
    gate_proj = centred(key_list[11], (D, FF), D ** -0.5, 0.125, ((0, 4), (1, 4)), jnp.float32)
    up_scales = jnp.clip(jnp.exp(math.log(2.0) - 1.3862944 * jax.random.uniform(key_list[12], (2, FF), jnp.float32) ** shard_levels(key_list[12], (2, FF), ((1, 4),), -0.2, 0.2)), 0.5, 2.0)
    ffn_taps = centred(key_list[13], (3, 2, FF), 3 ** -0.5, 3.5, ((2, 4),), jnp.float32)
    ffn_shift = centred(key_list[14], (2, FF), 0.5, 3.0, ((1, 4),), jnp.float32)
    down_proj = centred(key_list[15], (FF, D), FF ** -0.5, 0.109375, ((0, 4), (1, 4)), jnp.float32)
    down_scale = jnp.clip(jnp.exp(math.log(3.0) - 2.3025851 * jax.random.uniform(key_list[16], (D,), jnp.float32) ** shard_levels(key_list[16], (D,), ((0, 4),), -0.2, 0.2)), 0.3, 3.0)
    second_gain = jnp.clip(1.0 + 0.18 * jax.random.normal(key_list[17], (D,), jnp.float32), 0.1, 1.9)
    second_shift = centred(key_list[18], (D,), 0.3, 2.0, (), jnp.float32)
    return {"tokens": tokens, "outer_gate": outer_gate, "inner_gate": inner_gate, "mixer_value": mixer_value, "mixer_scales": mixer_scales, "mixer_taps": mixer_taps, "mixer_out": mixer_out, "out_scale": out_scale, "first_gain": first_gain, "first_shift": first_shift, "up_proj": up_proj, "gate_proj": gate_proj, "up_scales": up_scales, "ffn_taps": ffn_taps, "ffn_shift": ffn_shift, "down_proj": down_proj, "down_scale": down_scale, "second_gain": second_gain, "second_shift": second_shift}


norm_eps = 1e-05
residual_weight = 8.0 ** 0.25

def causal_mix(signal, kernel_taps):
    sequences = signal.reshape(-1, LEN, signal.shape[-1])
    padded = jnp.pad(sequences, ((0, 0), (2, 0), (0, 0)))
    mixed = kernel_taps[0] * padded[:, :-2] + kernel_taps[1] * padded[:, 1:-1] + kernel_taps[2] * padded[:, 2:]
    return mixed.reshape(signal.shape)

def layer_norm(summed, gain_vector, shift_vector):
    average = lax.optimization_barrier(jnp.mean(summed, -1, keepdims=True))
    spread = lax.optimization_barrier(jnp.mean(jnp.square(summed - average), -1, keepdims=True))
    return (summed - average) * lax.rsqrt(spread + norm_eps) * gain_vector + shift_vector

def lowered(matrix):
    return matrix.astype(jnp.bfloat16)

def project(left_rows, matrix, column_scale):
    return jnp.dot(left_rows, lowered(matrix), preferred_element_type=jnp.float32) * column_scale

def reference(tokens, outer_gate, inner_gate, mixer_value, mixer_scales, mixer_taps, mixer_out, out_scale, first_gain, first_shift, up_proj, gate_proj, up_scales, ffn_taps, ffn_shift, down_proj, down_scale, second_gain, second_shift):
    outer_part = project(tokens, outer_gate, mixer_scales[0]).astype(jnp.bfloat16)
    inner_part = project(tokens, inner_gate, mixer_scales[1]).astype(jnp.bfloat16)
    value_part = project(tokens, mixer_value, mixer_scales[2]).astype(jnp.bfloat16)
    product = inner_part.astype(jnp.float32) * value_part.astype(jnp.float32)
    mixed_conv = (outer_part.astype(jnp.float32) * causal_mix(product, mixer_taps)).astype(jnp.bfloat16)
    mixer_sum = project(mixed_conv, mixer_out, out_scale)
    first_sum = residual_weight * tokens.astype(jnp.float32) + mixer_sum
    normed = layer_norm(first_sum, first_gain, first_shift).astype(jnp.bfloat16)
    up_linear = project(normed, up_proj, up_scales[0])
    gate_linear = project(normed, gate_proj, up_scales[1])
    up_mixed = causal_mix(up_linear, ffn_taps[:, 0]) + ffn_shift[0]
    gate_mixed = causal_mix(gate_linear, ffn_taps[:, 1]) + ffn_shift[1]
    hidden = (up_mixed * jax.nn.silu(gate_mixed)).astype(jnp.bfloat16)
    ffn_sum = project(hidden, down_proj, down_scale)
    second_sum = residual_weight * normed.astype(jnp.float32) + ffn_sum
    return layer_norm(second_sum, second_gain, second_shift).astype(jnp.bfloat16)
```

```python
import jax
import jax.numpy as jnp
from jax import lax
from jax.sharding import PartitionSpec as P

LEN = 128


norm_eps = 1e-05
residual_weight = 8.0**0.25


def causal_mix(signal, kernel_taps):
    sequences = signal.reshape(-1, LEN, signal.shape[-1])
    padded = jnp.pad(sequences, ((0, 0), (2, 0), (0, 0)))
    mixed = (
        kernel_taps[0] * padded[:, :-2]
        + kernel_taps[1] * padded[:, 1:-1]
        + kernel_taps[2] * padded[:, 2:]
    )
    return mixed.reshape(signal.shape)


def lowered(matrix):
    return matrix.astype(jnp.bfloat16)


def halves(extent, unit):
    square = lax.axis_size("fs") == lax.axis_size("tp")
    return square and lax.axis_size("rep") == 2 and extent % (2 * unit) == 0


def shift(array, axis, distance, wrap):
    count = lax.axis_size(axis)
    pairs = [
        (place, (place + distance) % count)
        for place in range(count)
        if wrap or 0 <= place + distance < count
    ]
    return lax.ppermute(array, axis, pairs)


def twin(array, axis, mask):
    return lax.ppermute(array, axis, [(place, place ^ mask) for place in range(lax.axis_size(axis))])


def ring_blocks(piece):
    count = lax.axis_size("fs")
    if count == 4:
        across = shift(piece, "fs", 2, True)
        ahead = shift(piece, "fs", 1, False) + lax.ppermute(across, "fs", [(1, 0)])
        behind = shift(piece, "fs", -1, False) + lax.ppermute(across, "fs", [(2, 3)])
        return [piece, ahead, across, behind]
    whole = lax.all_gather(piece, "fs", axis=0)
    own = lax.axis_index("fs")
    return [
        lax.dynamic_index_in_dim(whole, (own - k) % count, 0, keepdims=False) for k in range(count)
    ]


def weight_blocks(shard, axis, unit):
    if not halves(shard.shape[axis], unit):
        return [(block,) for block in ring_blocks(lowered(shard))]
    extent = shard.shape[axis] // 2
    rep = lax.axis_index("rep")
    mine = lowered(lax.dynamic_slice_in_dim(shard, rep * extent, extent, axis))
    other = lowered(lax.dynamic_slice_in_dim(shard, (1 - rep) * extent, extent, axis))
    blocks = ring_blocks(mine)
    return [(mine, other)] + [(block, twin(block, "rep", 1)) for block in blocks[1:]]


def half_vectors(vector, parts):
    if parts == 1:
        return [vector]
    extent = vector.shape[-1] // 2
    rep = lax.axis_index("rep")
    return [
        lax.dynamic_slice_in_dim(vector, place * extent, extent, vector.ndim - 1)
        for place in (rep, 1 - rep)
    ]


def channel_blocks(piece):
    count = lax.axis_size("tp")
    if count & (count - 1):
        whole = lax.all_gather(piece, "tp", axis=0)
        own = lax.axis_index("tp")
        return jnp.stack([whole[(own + m) % count] for m in range(count)])
    found = {0: piece}
    mask = count // 2
    while mask:
        for place in list(found):
            found[place ^ mask] = twin(found[place], "tp", mask)
        mask //= 2
    return jnp.stack([found[m] for m in range(count)])


def member_block(blocks, member):
    count = lax.axis_size("tp")
    own = lax.axis_index("tp")
    place = (member - own) % count if count & (count - 1) else member ^ own
    return lax.dynamic_index_in_dim(blocks, place, 0, keepdims=False)


def contracted(blocks, k, weight_rows):
    fs = lax.axis_size("fs")
    tp = lax.axis_size("tp")
    member = (lax.axis_index("fs") - k) % fs
    if fs == tp:
        return member_block(blocks, member)
    width = blocks.shape[-1]
    start = member * weight_rows
    if weight_rows <= width:
        block = member_block(blocks, start // width)
        return lax.dynamic_slice_in_dim(block, start % width, weight_rows, 1)
    return jnp.concatenate(
        [member_block(blocks, start // width + n) for n in range(weight_rows // width)], axis=1
    )


def add_dot(total, operand, weight):
    partial = jnp.dot(operand, weight, preferred_element_type=jnp.float32)
    return partial if total is None else total + partial


def row_stats(summed):
    stats = jnp.stack([jnp.sum(summed, 1), jnp.sum(summed * summed, 1)])
    count = lax.axis_size("tp")
    if count & (count - 1):
        stats = lax.psum(stats, "tp")
    else:
        mask = 1
        while mask < count:
            stats = stats + twin(stats, "tp", mask)
            mask *= 2
    return stats[0][:, None], stats[1][:, None]


def own_columns(vector, own_width):
    return lax.dynamic_slice_in_dim(vector, lax.axis_index("tp") * own_width, own_width, 0)


def scaled_norm(summed, average, spread, gain_vector, shift_vector):
    return (summed - average) * lax.rsqrt(spread + norm_eps) * gain_vector + shift_vector


def local(
    tokens,
    outer_gate,
    inner_gate,
    mixer_value,
    mixer_scales,
    mixer_taps,
    mixer_out,
    out_scale,
    first_gain,
    first_shift,
    up_proj,
    gate_proj,
    up_scales,
    ffn_taps,
    ffn_shift,
    down_proj,
    down_scale,
    second_gain,
    second_shift,
):
    own_width = tokens.shape[1]
    full_width = own_width * lax.axis_size("tp")
    gates = weight_blocks(jnp.concatenate([outer_gate, inner_gate, mixer_value], axis=1), 0, 128)
    outs = weight_blocks(mixer_out, 1, 128)
    ups = weight_blocks(up_proj, 1, 128)
    gate_ups = weight_blocks(gate_proj, 1, 128)
    downs = weight_blocks(down_proj, 0, 128)
    rep = lax.axis_index("rep")

    token_blocks = channel_blocks(tokens)
    total = None
    for k, parts in enumerate(gates):
        rows = sum(part.shape[0] for part in parts)
        operand = contracted(token_blocks, k, rows)
        for n, part in enumerate(parts):
            if len(parts) == 1:
                piece = operand
            else:
                start = (rep if n == 0 else 1 - rep) * part.shape[0]
                piece = lax.dynamic_slice_in_dim(operand, start, part.shape[0], 1)
            total = add_dot(total, piece, part)
    outer_part, inner_part, value_part = jnp.split(total, 3, axis=1)
    outer_part = (outer_part * mixer_scales[0]).astype(jnp.bfloat16)
    inner_part = (inner_part * mixer_scales[1]).astype(jnp.bfloat16)
    value_part = (value_part * mixer_scales[2]).astype(jnp.bfloat16)
    product = inner_part.astype(jnp.float32) * value_part.astype(jnp.float32)
    mixed_conv = (outer_part.astype(jnp.float32) * causal_mix(product, mixer_taps)).astype(
        jnp.bfloat16
    )
    conv_blocks = channel_blocks(mixed_conv)
    columns = [None] * len(outs[0])
    for k, parts in enumerate(outs):
        operand = contracted(conv_blocks, k, parts[0].shape[0])
        for n, part in enumerate(parts):
            columns[n] = add_dot(columns[n], operand, part)
    if len(columns) == 1:
        mixer_sum = columns[0]
    else:
        mixer_sum = jnp.where(
            rep == 0,
            jnp.concatenate(columns, axis=1),
            jnp.concatenate(columns[::-1], axis=1),
        )
    first_sum = residual_weight * tokens.astype(jnp.float32) + mixer_sum * out_scale
    row_total, row_square = row_stats(first_sum)
    average = row_total / full_width
    spread = row_square / full_width - average * average
    normed = scaled_norm(
        first_sum,
        average,
        spread,
        own_columns(first_gain, own_width),
        own_columns(first_shift, own_width),
    ).astype(jnp.bfloat16)
    normed_blocks = channel_blocks(normed)
    operands = [contracted(normed_blocks, k, up_proj.shape[0]) for k in range(len(ups))]
    count = len(ups[0])
    scales = half_vectors(up_scales, count)
    taps = half_vectors(ffn_taps, count)
    shifts = half_vectors(ffn_shift, count)
    hidden_blocks = []
    for n in range(count):
        up_linear = gate_linear = None
        for k, operand in enumerate(operands):
            up_linear = add_dot(up_linear, operand, ups[k][n])
            gate_linear = add_dot(gate_linear, operand, gate_ups[k][n])
        up_linear = up_linear * scales[n][0]
        gate_linear = gate_linear * scales[n][1]
        up_mixed = causal_mix(up_linear, taps[n][:, 0]) + shifts[n][0]
        gate_mixed = causal_mix(gate_linear, taps[n][:, 1]) + shifts[n][1]
        hidden = (up_mixed * jax.nn.silu(gate_mixed)).astype(jnp.bfloat16)
        hidden_blocks.append(channel_blocks(hidden))
    ffn_sum = None
    for n in range(count):
        for k, parts in enumerate(downs):
            operand = contracted(hidden_blocks[n], k, parts[n].shape[0])
            ffn_sum = add_dot(ffn_sum, operand, parts[n])
    second_sum = residual_weight * normed.astype(jnp.float32) + ffn_sum * down_scale
    second_total, second_square = row_stats(second_sum)
    second_average = second_total / full_width
    second_spread = second_square / full_width - second_average * second_average
    return scaled_norm(
        second_sum,
        second_average,
        second_spread,
        own_columns(second_gain, own_width),
        own_columns(second_shift, own_width),
    ).astype(jnp.bfloat16)


def solution(mesh):
    return jax.shard_map(
        local,
        mesh=mesh,
        in_specs=(
            P(("rep", "fs"), "tp"),
            P("fs", "tp"),
            P("fs", "tp"),
            P("fs", "tp"),
            P(None, "tp"),
            P(None, "tp"),
            P("fs", "tp"),
            P("tp"),
            P(),
            P(),
            P("fs", "tp"),
            P("fs", "tp"),
            P(None, "tp"),
            P(None, None, "tp"),
            P(None, "tp"),
            P("fs", "tp"),
            P("tp"),
            P(),
            P(),
        ),
        out_specs=P(("rep", "fs"), "tp"),
        check_vma=False,
    )
```
